256 devices in a mesh: rep: 2 (over z_hi), fs: 16 (over z_lo, y), tp: 8 (over x, core).
Axes of the slice: x: 4, y: 4, z: 8 (z_hi: 2, z_lo: 4; z = z_hi * 4 + z_lo), core: 2. Of those that a mesh axis runs over, the one named last changes fastest.
Arguments:
- tokens: bfloat16 [16384, 2048], P(('rep', 'fs'), 'tp'), may hold values from -6 to 6
- pre_gain: float32 [2048], replicated, may hold values from 0.1 to 1.9
- u_weight: float32 [2048, 512], P('fs', 'tp'), may hold values from -0.125 to 0.125
- u_scale: float32 [512], P('tp'), may hold values from 0.5 to 2
- v_weight: float32 [2048, 512], P('fs', 'tp'), may hold values from -0.125 to 0.125
- v_scale: float32 [512], P('tp'), may hold values from 0.5 to 2
- group_gain: float32 [512], P('tp'), may hold values from 0.1 to 1.9
- span_weight: bfloat16 [8, 128, 128], P('tp'), may hold values from -0.5 to 0.5
- span_bias: float32 [8, 128], P('tp'), may hold values from 0.5 to 1.5
- out_weight: float32 [512, 2048], P('tp', 'fs'), may hold values from -0.25 to 0.25
- out_scale: float32 [2048], P('fs'), may hold values from 0.5 to 2
- ffn_gain: float32 [2048], replicated, may hold values from 0.1 to 1.9
- gate_weight: float32 [2048, 5632], P('fs', 'tp'), may hold values from -0.125 to 0.125
- gate_scale: float32 [5632], P('tp'), may hold values from 0.5 to 2
- up_weight: float32 [2048, 5632], P('fs', 'tp'), may hold values from -0.125 to 0.125
- up_scale: float32 [5632], P('tp'), may hold values from 0.5 to 2
- down_weight: float32 [5632, 2048], P('tp', 'fs'), may hold values from -0.078125 to 0.078125
- down_scale: float32 [2048], P('fs'), may hold values from 0.5 to 2
Outputs:
- layer_out: bfloat16 [16384, 2048], P(('rep', 'fs'), 'tp')
The draws below stay inside these ranges and needn't reach their ends.
All inputs are finite; a program needn't handle non-finite values.
Results may differ from the reference program's by a relative error of at most 0.02.
Values may be sent and summed in bfloat16 or wider, within the bound.
No kernel may reach another device: no remote copies, remote signals or barrier semaphores. Data moves between devices by JAX's collectives and lax.ppermute only.
A program may use at most 64 MiB of HBM per device.

```python
import math
import jax
import jax.numpy as jnp
from jax import lax

D = 2048
GROUPS = 8
GROUP_DIM = 64
MIX_WIDTH = 512
HIDDEN_SIZE = 5632
SPAN = 128
TOKENS = 16384
N_TP = 8


def levels(rng, shape, shards, smallest, largest):
    def one(dim, shards_of):
        steps = jax.random.uniform(jax.random.fold_in(jax.random.fold_in(rng, 6), dim), (shards_of,), jnp.float32, smallest / len(shards), largest / len(shards))
        return jnp.repeat(jnp.exp(steps), shape[dim] // shards_of).reshape((-1,) + (1,) * (len(shape) - dim - 1))

    level = one(*shards[0])
    for cut in shards[1:]:
        level = level * one(*cut)
    return level


def normal_values(key, extent, scale, reach, shards=(), held_as=jnp.bfloat16):
    entries = jax.random.normal(key, extent, jnp.float32) * scale
    if len(shards) > 0:
        entries = levels(key, extent, shards, -0.22, 0.18) * entries
    return jnp.clip(entries, min=-reach, max=reach).astype(held_as)


def setup_inputs(seed: int = 0) -> dict:
    arg_keys = jax.random.split(jax.random.key(seed), 19)
    tokens = normal_values(arg_keys[0], (TOKENS, D), 1.0, 6.0, ((0, 32), (1, 8)))
    pre_gain = jnp.clip(1.0 + 0.18 * jax.random.normal(arg_keys[1], (D,), jnp.float32), 0.1, 1.9)
    u_weight = normal_values(arg_keys[2], (D, MIX_WIDTH), D ** -0.5, 0.125, ((0, 16), (1, 8)), jnp.float32)
    u_scale = jnp.clip(jnp.exp(math.log(2.0) - 1.3862944 * jax.random.uniform(arg_keys[3], (MIX_WIDTH,), jnp.float32) ** levels(arg_keys[3], (MIX_WIDTH,), ((0, 8),), -0.2, 0.2)), 0.5, 2.0)
    v_weight = normal_values(arg_keys[4], (D, MIX_WIDTH), D ** -0.5, 0.125, ((0, 16), (1, 8)), jnp.float32)
    v_scale = jnp.clip(jnp.exp(math.log(2.0) - 1.3862944 * jax.random.uniform(arg_keys[5], (MIX_WIDTH,), jnp.float32) ** levels(arg_keys[5], (MIX_WIDTH,), ((0, 8),), -0.2, 0.2)), 0.5, 2.0)
    group_gain = jnp.clip(1.0 + 0.18 * jax.random.normal(arg_keys[6], (MIX_WIDTH,), jnp.float32), 0.1, 1.9)
    span_weight = normal_values(arg_keys[7], (GROUPS, SPAN, SPAN), SPAN ** -0.5, 0.5, ((0, 8),))
    span_bias = jnp.clip(0.5 + 1.0 * jax.random.uniform(arg_keys[8], (GROUPS, SPAN), jnp.float32) ** levels(arg_keys[8], (GROUPS, SPAN), ((0, 8),), -0.2, 0.2), 0.5, 1.5)
    out_weight = normal_values(arg_keys[9], (MIX_WIDTH, D), MIX_WIDTH ** -0.5, 0.25, ((0, 8), (1, 16)), jnp.float32)
    out_scale = jnp.clip(jnp.exp(math.log(2.0) - 1.3862944 * jax.random.uniform(arg_keys[10], (D,), jnp.float32) ** levels(arg_keys[10], (D,), ((0, 16),), -0.2, 0.2)), 0.5, 2.0)
    ffn_gain = jnp.clip(1.0 + 0.18 * jax.random.normal(arg_keys[11], (D,), jnp.float32), 0.1, 1.9)
    gate_weight = normal_values(arg_keys[12], (D, HIDDEN_SIZE), D ** -0.5, 0.125, ((0, 16), (1, 8)), jnp.float32)
    gate_scale = jnp.clip(jnp.exp(math.log(2.0) - 1.3862944 * jax.random.uniform(arg_keys[13], (HIDDEN_SIZE,), jnp.float32) ** levels(arg_keys[13], (HIDDEN_SIZE,), ((0, 8),), -0.2, 0.2)), 0.5, 2.0)
    up_weight = normal_values(arg_keys[14], (D, HIDDEN_SIZE), D ** -0.5, 0.125, ((0, 16), (1, 8)), jnp.float32)
    up_scale = jnp.clip(jnp.exp(math.log(2.0) - 1.3862944 * jax.random.uniform(arg_keys[15], (HIDDEN_SIZE,), jnp.float32) ** levels(arg_keys[15], (HIDDEN_SIZE,), ((0, 8),), -0.2, 0.2)), 0.5, 2.0)
    down_weight = normal_values(arg_keys[16], (HIDDEN_SIZE, D), HIDDEN_SIZE ** -0.5, 0.078125, ((0, 8), (1, 16)), jnp.float32)
    down_scale = jnp.clip(jnp.exp(math.log(2.0) - 1.3862944 * jax.random.uniform(arg_keys[17], (D,), jnp.float32) ** levels(arg_keys[17], (D,), ((0, 16),), -0.2, 0.2)), 0.5, 2.0)
    return {"tokens": tokens, "pre_gain": pre_gain, "u_weight": u_weight, "u_scale": u_scale, "v_weight": v_weight, "v_scale": v_scale, "group_gain": group_gain, "span_weight": span_weight, "span_bias": span_bias, "out_weight": out_weight, "out_scale": out_scale, "ffn_gain": ffn_gain, "gate_weight": gate_weight, "gate_scale": gate_scale, "up_weight": up_weight, "up_scale": up_scale, "down_weight": down_weight, "down_scale": down_scale}


EPS = 0.02

def rms_rows(values, gain):
    wide = values.astype(jnp.float32)
    scaled = wide * lax.rsqrt(lax.optimization_barrier(jnp.mean(wide * wide, axis=-1, keepdims=True)) + EPS)
    return (scaled * gain).astype(jnp.bfloat16)

def block_sum(acts, weight, scale):
    width = acts.shape[1] // N_TP
    acts_blocks = jnp.moveaxis(acts.reshape(acts.shape[0], N_TP, width), 1, 0)
    weight_blocks = weight.astype(jnp.bfloat16).reshape(N_TP, width, weight.shape[1])

    def add_block(total, pair):
        term = (jnp.dot(pair[0], pair[1], preferred_element_type=jnp.float32) * scale).astype(jnp.bfloat16)
        return (total + term.astype(jnp.float32), None)
    start = jnp.zeros((acts.shape[0], weight.shape[1]), jnp.float32)
    total, unused = lax.scan(add_block, start, (acts_blocks, weight_blocks))
    return total.astype(jnp.bfloat16)

def reference(tokens, pre_gain, u_weight, u_scale, v_weight, v_scale, group_gain, span_weight, span_bias, out_weight, out_scale, ffn_gain, gate_weight, gate_scale, up_weight, up_scale, down_weight, down_scale):
    row_count = tokens.shape[0]
    normed = rms_rows(tokens, pre_gain)
    u_act = jax.nn.gelu(jnp.dot(normed, u_weight.astype(jnp.bfloat16), preferred_element_type=jnp.float32) * u_scale)
    v_act = jax.nn.gelu(jnp.dot(normed, v_weight.astype(jnp.bfloat16), preferred_element_type=jnp.float32) * v_scale)
    grouped = v_act.reshape(row_count, GROUPS, GROUP_DIM)
    centre = lax.optimization_barrier(jnp.mean(grouped, axis=-1, keepdims=True))
    spread = lax.optimization_barrier(jnp.mean(jnp.square(grouped - centre), axis=-1, keepdims=True))
    v_norm = (((grouped - centre) * lax.rsqrt(spread + EPS)).reshape(row_count, MIX_WIDTH) * group_gain).astype(jnp.bfloat16)
    spans = v_norm.reshape(row_count // SPAN, SPAN, GROUPS, GROUP_DIM).astype(jnp.float32)
    lower = jnp.tril(span_weight).astype(jnp.float32)
    mixed = jnp.einsum('gts,nsgc->ntgc', lower, spans) + jnp.transpose(span_bias)[None, :, :, None]
    gated = (u_act * mixed.reshape(row_count, MIX_WIDTH)).astype(jnp.bfloat16)
    mix = (jnp.dot(gated, out_weight.astype(jnp.bfloat16), preferred_element_type=jnp.float32) * out_scale).astype(jnp.bfloat16)
    resid = (tokens.astype(jnp.float32) + mix.astype(jnp.float32)).astype(jnp.bfloat16)
    normed_ffn = rms_rows(resid, ffn_gain)
    gate_pre = jnp.dot(normed_ffn, gate_weight.astype(jnp.bfloat16), preferred_element_type=jnp.float32) * gate_scale
    up_pre = jnp.dot(normed_ffn, up_weight.astype(jnp.bfloat16), preferred_element_type=jnp.float32) * up_scale
    hidden = (jax.nn.silu(gate_pre) * up_pre).astype(jnp.bfloat16)
    ffn = block_sum(hidden, down_weight, down_scale)
    return (resid.astype(jnp.float32) + ffn.astype(jnp.float32)).astype(jnp.bfloat16)
```

```python
import jax
import jax.numpy as jnp
from jax import lax
from jax.experimental import pallas as pl
from jax.experimental.pallas import tpu as pltpu
from jax.sharding import Mesh
from jax.sharding import PartitionSpec as P

EPS = 0.02
BF = jnp.bfloat16
F32 = jnp.float32
NT = (((1,), (1,)), ((), ()))

AXES = ("zh", "zl", "y", "x", "c")
FIRST = (("ye", "yo", "ze", "zo"), ("ze", "zo", "ye", "yo"))
SECOND = (("yo", "ye", "zo", "ze"), ("zo", "ze", "yo", "ye"))
ALONG = (("xe", "xo"), ("xo", "xe"))


def over(kind, v, size):
    if kind == "e":
        return v ^ 1
    return (v + 2 * (v & 1) - 1) % size


def exchange(array, edges):
    pairs = []
    for i in range(256):
        place = {"z": i // 32, "y": i // 8 % 4, "x": i // 2 % 4, "c": i % 2}
        edge = edges[place["c"]]
        if edge == "c":
            place["c"] ^= 1
        else:
            axis = edge[0]
            place[axis] = over(edge[1], place[axis], 8 if axis == "z" else 4)
        j = ((place["z"] * 4 + place["y"]) * 4 + place["x"]) * 2 + place["c"]
        pairs.append((i, j))
    return lax.ppermute(array, AXES, pairs)


def grown(array, orders, steps):
    for s in steps:
        got = exchange(array, (orders[0][s], orders[1][s]))
        array = jnp.concatenate([array, got], axis=0)
    return array


def swapped(array):
    return exchange(array, ("c", "c"))


def hop(kind, v):
    return over(kind, v, 4) if kind == "e" else (v + 2 * (v & 1) - 1) & 3


def source(order, position, place):
    place = dict(place)
    for s in reversed(range(len(order))):
        if position >> s & 1:
            axis = order[s][0]
            place[axis] = hop(order[s][1], place[axis])
    return place


def position(order, place, target):
    found = 0
    for axis in target:
        kinds = [(s, e[1]) for s, e in enumerate(order) if e[0] == axis]
        here, there = place[axis], target[axis]
        odd = ((there ^ here) >> 1) & 1
        if kinds[1][1] == "o":
            even = (jnp.where(odd == 1, hop("o", here), here) ^ there) & 1
        else:
            even = (jnp.where(odd == 1, hop("o", there), there) ^ here) & 1
        for s, kind in kinds:
            found = found + ((odd if kind == "o" else even) << s)
    return found


def by_core(c, of):
    zero, one = of(0), of(1)
    if isinstance(zero, dict):
        return {a: jnp.where(c == 0, zero[a], one[a]) for a in zero}
    return jnp.where(c == 0, zero, one)


def squares(values):
    wide = values.astype(F32)
    wide = wide * wide
    return wide[:, :128] + wide[:, 128:]


def here(at):
    return {"x": at[0], "y": at[1], "z": at[2]}, at[3]


def blocks_of(at):
    place, c = here(at)
    for p in range(4):
        for part in range(2):
            ct = c if part == 0 else 1 - c
            yield p, part, by_core(ct, lambda k: source(ALONG[k], p, {"x": place["x"]})["x"]), ct


def mixer_kernel(at, own, other, small, gain, u_scale, v_scale, group_gain, span, bias, gated):
    place, c = here(at)
    tokens = (own, other)
    lanes = jnp.zeros((own.shape[1], 128), F32)
    for p in range(4):
        for part in range(2):
            lanes += squares(tokens[part][p])
    inverse = lax.rsqrt(jnp.sum(lanes, axis=-1, keepdims=True) * (1.0 / 2048) + EPS)
    sums = jnp.zeros((own.shape[1], 128), F32)
    for p, part, xt, ct in blocks_of(at):
        row = jnp.concatenate(
            [gain[pl.ds(4 * xt + 2 * ct, 1), :], gain[pl.ds(4 * xt + 2 * ct + 1, 1), :]], axis=-1
        )
        normed = (tokens[part][p].astype(F32) * inverse * row).astype(BF)
        pieces = []
        for h in range(2):
            target = {"y": 2 * ct + h, "z": xt}
            pieces.append(small[by_core(c, lambda k: position(FIRST[k], place, target)), :128, :])
        weights = jnp.concatenate(pieces, axis=-1)
        sums += lax.dot_general(normed, weights, NT, preferred_element_type=F32)
    acts = jax.nn.gelu(sums * jnp.concatenate([u_scale[...], v_scale[...]], axis=-1))
    u_act = acts[:, :64]
    v_act = acts[:, 64:]
    centred = v_act - jnp.mean(v_act, axis=-1, keepdims=True)
    spread = jnp.mean(centred * centred, axis=-1, keepdims=True)
    v_norm = (centred * lax.rsqrt(spread + EPS) * group_gain[...]).astype(BF)
    t = lax.broadcasted_iota(jnp.int32, (128, 128), 0)
    s = lax.broadcasted_iota(jnp.int32, (128, 128), 1)
    lower = jnp.where(s <= t, span[0].astype(F32), 0.0).astype(BF)
    level = jnp.sum(jnp.where(s == t, bias[...], 0.0), axis=-1, keepdims=True)
    for n in range(own.shape[1] // 128):
        rows = slice(n * 128, (n + 1) * 128)
        mixed = jnp.dot(lower, v_norm[rows], preferred_element_type=F32) + level
        gated[0, rows, :] = (u_act[rows] * mixed).astype(BF)


def out_kernel(at, own, other, g_own, g_other, o_own, o_other, gain, normed, resid, gates, weights):
    place, c = here(at)
    tokens = (own, other)
    for p in range(4):
        gates[:, 64 * p : 64 * p + 64] = g_own[p]
        gates[:, 256 + 64 * p : 256 + 64 * p + 64] = g_other[p]
    lanes = jnp.zeros((own.shape[1], 128), F32)
    for p, part, xt, ct in blocks_of(at):
        for h in range(2):
            target = {"y": 2 * ct + h, "z": xt}
            mine = by_core(c, lambda k: position(FIRST[k], place, target))
            theirs = by_core(1 - c, lambda k: position(FIRST[k], place, target))
            columns = slice(128 * h, 128 * h + 128)
            for j in range(4):
                weights[64 * j : 64 * j + 64, columns] = o_own[j, mine]
                weights[256 + 64 * j : 320 + 64 * j, columns] = o_other[j, theirs]
        mix = jnp.dot(gates[...], weights[...], preferred_element_type=F32).astype(BF)
        sums = (tokens[part][p].astype(F32) + mix.astype(F32)).astype(BF)
        lanes += squares(sums)
        f = 4 * xt + 2 * ct
        normed[f] = sums[:, :128]
        normed[f + 1] = sums[:, 128:]
        if p == 0 and part == 0:
            resid[...] = sums
    inverse = lax.rsqrt(jnp.sum(lanes, axis=-1, keepdims=True) * (1.0 / 2048) + EPS)
    for f in range(16):
        row = gain[f : f + 1, :]
        normed[f] = (normed[f].astype(F32) * inverse * row).astype(BF)


def add_terms(at, normed, weights, orders, base, acc, fresh):
    place, c = here(at)
    here_now = {"y": place["y"], "z": place["z"]}
    for pair in range(4):
        left = []
        for i in (2 * pair, 2 * pair + 1):
            src = by_core(c, lambda k: source(orders[k], base + i, here_now))
            left.append(normed[src["z"] * 4 + src["y"]])
        right = jnp.concatenate([weights[2 * pair], weights[2 * pair + 1]], axis=-1)
        term = lax.dot_general(
            jnp.concatenate(left, axis=-1), right, NT, preferred_element_type=F32
        )
        if fresh and pair == 0:
            acc[...] = term
        else:
            acc[...] += term


def early_kernel(at, normed, gate, up, gate_acc, up_acc):
    add_terms(at, normed, gate, FIRST, 0, gate_acc, True)
    add_terms(at, normed, up, SECOND, 0, up_acc, True)


def late_kernel(at, normed, gate, up, gate_acc, up_acc, g_scale, u_scale, hidden, sums):
    sums[0] = gate_acc[...]
    sums[1] = up_acc[...]
    add_terms(at, normed, gate, FIRST, 8, sums.at[0], False)
    add_terms(at, normed, up, SECOND, 8, sums.at[1], False)
    scaled = sums[0] * g_scale[...]
    hidden[...] = (scaled / (1.0 + jnp.exp(-scaled)) * (sums[1] * u_scale[...])).astype(BF)


def down_kernel(mine, at, hidden, low_0, low_1, high_0, high_1, sums, weights):
    place, c = here(at)
    ct = c if mine else 1 - c

    def fetch(index, refs, rows, columns):
        for half in range(2):

            @pl.when((index >> 3) == half)
            def _():
                weights[rows, columns] = refs[half][index & 7]

    for xt in range(4):
        for h in range(2):
            target = {"y": 2 * ct + h, "z": xt}
            columns = slice(128 * h, 128 * h + 128)
            low = by_core(c, lambda k: position(FIRST[k], place, target))
            high = by_core(c, lambda k: position(SECOND[k], place, target))
            fetch(low, (low_0, low_1), slice(0, 352), columns)
            fetch(high, (high_0, high_1), slice(352, 704), columns)
        term = jnp.dot(hidden[...], weights[...], preferred_element_type=F32).astype(BF)

        def rank(k):
            first, second = ALONG[k][1][1], ALONG[k][0][1]
            x = place["x"]
            return jnp.where(
                xt == x,
                0,
                jnp.where(xt == hop(second, x), 1, jnp.where(xt == hop(first, x), 2, 3)),
            )

        r = by_core(ct, rank)
        sums[r, 0] = term[:, :128]
        sums[r, 1] = term[:, 128:]


def down_own(*refs):
    down_kernel(True, *refs)


def down_other(*refs):
    down_kernel(False, *refs)


VMEM = pl.BlockSpec(memory_space=pltpu.VMEM)
SMEM = pl.BlockSpec(memory_space=pltpu.SMEM)


def call(kernel, outs, count, flops, scratch=(), name=None):
    return pl.pallas_call(
        kernel,
        out_shape=outs,
        in_specs=[SMEM] + [VMEM] * (count - 1),
        out_specs=jax.tree.map(lambda _: VMEM, outs),
        scratch_shapes=list(scratch),
        compiler_params=pltpu.CompilerParams(vmem_limit_bytes=60 * 1024 * 1024),
        cost_estimate=pl.CostEstimate(flops=flops, bytes_accessed=1 << 22, transcendentals=0),
        name=name,
    )


def shards(
    tokens,
    pre_gain,
    u_weight,
    u_scale,
    v_weight,
    v_scale,
    group_gain,
    span_weight,
    span_bias,
    out_weight,
    out_scale,
    ffn_gain,
    gate_weight,
    gate_scale,
    up_weight,
    up_scale,
    down_weight,
    down_scale,
):
    shape = jax.ShapeDtypeStruct
    rows = tokens.shape[0]
    at = jnp.stack([lax.axis_index(n) for n in ("x", "y", "zl", "c")]).astype(jnp.int32)

    tok_own = grown(tokens[None], ALONG, (0, 1))
    tok_other = swapped(tok_own)

    out_scaled = (out_weight.astype(BF).astype(F32) * out_scale).astype(BF)
    down_scaled = (down_weight.astype(BF).astype(F32) * down_scale).astype(BF)
    small = jnp.concatenate([u_weight.T.astype(BF), v_weight.T.astype(BF), out_scaled], axis=0)
    small = grown(small[None], FIRST, (0, 1, 2, 3))

    first = jnp.concatenate([gate_weight.T.astype(BF), down_scaled[:352]], axis=0)[None]
    second = jnp.concatenate([up_weight.T.astype(BF), down_scaled[352:]], axis=0)[None]
    weights = []
    for array, orders in ((first, FIRST), (second, SECOND)):
        array = grown(array, orders, (0, 1))
        got = exchange(array, (orders[0][2], orders[1][2]))
        wide = jnp.concatenate([array[:, :704], got[:, :704]], axis=0)
        deep = jnp.concatenate([array[:, 704:], got[:, 704:]], axis=0)
        last = (orders[0][3], orders[1][3])
        weights.append((wide, exchange(wide, last), deep, exchange(deep, last)))
    (gate_0, gate_1, low_0, low_1), (up_0, up_1, high_0, high_1) = weights

    out_own = grown(small[None, :, 128:, :], ALONG, (0, 1))
    out_other = swapped(out_own)

    gated = call(mixer_kernel, shape((1, rows, 64), BF), 10, 3 * 10**8, name="mixer")(
        at,
        tok_own,
        tok_other,
        small,
        pre_gain.reshape(16, 128),
        u_scale.reshape(1, 64),
        v_scale.reshape(1, 64),
        group_gain.reshape(1, 64),
        span_weight,
        span_bias,
    )
    gated_own = grown(gated, ALONG, (0, 1))
    gated_other = swapped(gated_own)
    normed, resid = call(
        out_kernel,
        (shape((16, rows, 128), BF), shape((rows, 256), BF)),
        8,
        10**9,
        scratch=[pltpu.VMEM((rows, 512), BF), pltpu.VMEM((512, 256), BF)],
        name="out",
    )(at, tok_own, tok_other, gated_own, gated_other, out_own, out_other, ffn_gain.reshape(16, 128))
    accs = call(
        early_kernel, (shape((rows, 704), F32), shape((rows, 704), F32)), 4, 15 * 10**8, name="early"
    )(at, normed, gate_0, up_0)
    hidden = call(
        late_kernel,
        shape((rows, 704), BF),
        8,
        15 * 10**8,
        scratch=[pltpu.VMEM((2, rows, 704), F32)],
        name="late",
    )(at, normed, gate_1, up_1, *accs, gate_scale.reshape(1, 704), up_scale.reshape(1, 704))

    def down(kernel):
        return call(
            kernel,
            shape((4, 2, rows, 128), BF),
            6,
            75 * 10**7,
            scratch=[pltpu.VMEM((704, 256), BF)],
            name=kernel.__name__,
        )(at, hidden, low_0, low_1, high_0, high_1)

    theirs = swapped(down(down_other)).astype(F32)
    mine = down(down_own).astype(F32)
    sent = (mine[2:] + theirs[2:]).astype(BF)
    got = exchange(sent, (ALONG[0][1], ALONG[1][1])).astype(F32)
    sent = (mine[1] + theirs[1] + got[1]).astype(BF)
    ffn = mine[0] + theirs[0] + got[0] + exchange(sent, (ALONG[0][0], ALONG[1][0])).astype(F32)
    ffn = ffn.astype(BF).astype(F32)
    ffn = jnp.concatenate([ffn[0], ffn[1]], axis=-1)
    return (resid.astype(F32) + ffn).astype(BF)


def solution(mesh):
    torus = Mesh(mesh.devices.reshape(2, 4, 4, 4, 2), AXES)
    seq, fs, tp = ("zh", "zl", "y"), ("zl", "y"), ("x", "c")
    placed = (
        P(seq, tp),
        P(),
        P(fs, tp),
        P(tp),
        P(fs, tp),
        P(tp),
        P(tp),
        P(tp, None, None),
        P(tp, None),
        P(tp, fs),
        P(fs),
        P(),
        P(fs, tp),
        P(tp),
        P(fs, tp),
        P(tp),
        P(tp, fs),
        P(fs),
    )
    return jax.shard_map(
        shards, mesh=torus, in_specs=placed, out_specs=P(seq, tp), check_vma=False
    )
```

```python
import functools

import jax
import jax.numpy as jnp
from jax import lax
from jax.experimental import pallas as pl
from jax.experimental.pallas import tpu as pltpu
from jax.sharding import Mesh
from jax.sharding import PartitionSpec as P


EPS = 0.02
BF = jnp.bfloat16
F32 = jnp.float32
NT = (((1,), (1,)), ((), ()))
LOW = 352
PARTS = 2

AXES = ("zh", "zl", "y", "x", "c")
FIRST = (("ye", "yo", "ze", "zo"), ("ze", "zo", "ye", "yo"))
SECOND = (("yo", "ye", "zo", "ze"), ("zo", "ze", "yo", "ye"))
SMALL = (FIRST[1], FIRST[0])
ALONG = (("xe", "xo"), ("xo", "xe"))


def over(kind, v, size):
    if kind == "e":
        return v ^ 1
    return (v + 2 * (v & 1) - 1) % size


def exchange(array, edges):
    pairs = []
    for i in range(256):
        place = {"z": i // 32, "y": i // 8 % 4, "x": i // 2 % 4, "c": i % 2}
        edge = edges[place["c"]]
        if edge == "c":
            place["c"] ^= 1
        else:
            axis = edge[0]
            place[axis] = over(edge[1], place[axis], 8 if axis == "z" else 4)
        j = ((place["z"] * 4 + place["y"]) * 4 + place["x"]) * 2 + place["c"]
        pairs.append((i, j))
    return lax.ppermute(array, AXES, pairs)


def grown(array, orders, steps):
    for s in steps:
        got = exchange(array, (orders[0][s], orders[1][s]))
        array = jnp.concatenate([array, got], axis=0)
    return array


def swapped(array):
    return exchange(array, ("c", "c"))


def hop(kind, v):
    return over(kind, v, 4) if kind == "e" else (v + 2 * (v & 1) - 1) & 3


def source(order, position, place):
    place = dict(place)
    for s in reversed(range(len(order))):
        if position >> s & 1:
            axis = order[s][0]
            place[axis] = hop(order[s][1], place[axis])
    return place


def position(order, place, target):
    found = 0
    for axis in target:
        kinds = [(s, e[1]) for s, e in enumerate(order) if e[0] == axis]
        here, there = place[axis], target[axis]
        odd = ((there ^ here) >> 1) & 1
        if kinds[1][1] == "o":
            even = (jnp.where(odd == 1, hop("o", here), here) ^ there) & 1
        else:
            even = (jnp.where(odd == 1, hop("o", there), there) ^ here) & 1
        for s, kind in kinds:
            found = found + ((odd if kind == "o" else even) << s)
    return found


def by_core(c, of):
    zero, one = of(0), of(1)
    if isinstance(zero, dict):
        return {a: jnp.where(c == 0, zero[a], one[a]) for a in zero}
    return jnp.where(c == 0, zero, one)


def squares(values):
    wide = values.astype(F32)
    wide = wide * wide
    return wide[:, :128] + wide[:, 128:]


def here():
    return {"x": lax.axis_index("x"), "y": lax.axis_index("y"), "z": lax.axis_index("zl")}, lax.axis_index("c")


def blocks_of():
    place, c = here()
    for p in range(4):
        for part in range(2):
            ct = c if part == 0 else 1 - c
            yield p, part, by_core(ct, lambda k: source(ALONG[k], p, {"x": place["x"]})["x"]), ct


def mixer_kernel(own, other, small, gain, u_scale, v_scale, group_gain, span, bias, message):
    place, c = here()
    tokens = (own, other)
    lanes = jnp.zeros((own.shape[1], 128), F32)
    for p in range(4):
        for part in range(2):
            lanes += squares(tokens[part][p])
    inverse = lax.rsqrt(jnp.sum(lanes, axis=-1, keepdims=True) * (1.0 / 2048) + EPS)
    sums = jnp.zeros((own.shape[1], 128), F32)
    for p, part, xt, ct in blocks_of():
        row = jnp.concatenate(
            [gain[pl.ds(4 * xt + 2 * ct, 1), :], gain[pl.ds(4 * xt + 2 * ct + 1, 1), :]], axis=-1
        )
        normed = (tokens[part][p].astype(F32) * inverse * row).astype(BF)
        pieces = []
        for h in range(2):
            target = {"y": 2 * ct + h, "z": xt}
            pieces.append(small[by_core(c, lambda k: position(SMALL[k], place, target)), :128, :])
        weights = jnp.concatenate(pieces, axis=-1)
        sums += lax.dot_general(normed, weights, NT, preferred_element_type=F32)
    acts = jax.nn.gelu(sums * jnp.concatenate([u_scale[...], v_scale[...]], axis=-1))
    u_act = acts[:, :64]
    v_act = acts[:, 64:]
    centred = v_act - jnp.mean(v_act, axis=-1, keepdims=True)
    spread = jnp.mean(centred * centred, axis=-1, keepdims=True)
    v_norm = (centred * lax.rsqrt(spread + EPS) * group_gain[...]).astype(BF)
    t = lax.broadcasted_iota(jnp.int32, (128, 128), 0)
    s = lax.broadcasted_iota(jnp.int32, (128, 128), 1)
    for p in range(16):
        message[0, 64 * p : 64 * p + 64, :] = small[p, 128:, :]
    lower = jnp.where(s <= t, span[0].astype(F32), 0.0).astype(BF)
    level = jnp.sum(jnp.where(s == t, bias[...], 0.0), axis=-1, keepdims=True)
    for n in range(own.shape[1] // 128):
        rows = slice(n * 128, (n + 1) * 128)
        mixed = jnp.dot(lower, v_norm[rows], preferred_element_type=F32) + level
        low, side = 1024 + n % 2 * 128, 64 * (n // 2)
        message[0, low : low + 128, side : side + 64] = (u_act[rows] * mixed).astype(BF)


def out_kernel(own, other, m_own, m_other, gain, normed, resid, gates, weights):
    place, c = here()
    tokens = (own, other)
    for p in range(4):
        for part, message in enumerate((m_own, m_other)):
            side = 256 * part + 64 * p
            gates[:256, side : side + 64] = message[p, 1024:, :64]
            gates[256:, side : side + 64] = message[p, 1024:, 64:]
    lanes = jnp.zeros((own.shape[1], 128), F32)
    for p, part, xt, ct in blocks_of():
        for h in range(2):
            target = {"y": 2 * ct + h, "z": xt}
            mine = by_core(c, lambda k: position(SMALL[k], place, target))
            theirs = by_core(1 - c, lambda k: position(SMALL[k], place, target))
            columns = slice(128 * h, 128 * h + 128)
            for j in range(4):
                for base, message, found in ((0, m_own, mine), (256, m_other, theirs)):
                    block = message[j, pl.ds(pl.multiple_of(found * 64, 64), 64), :]
                    weights[base + 64 * j : base + 64 * j + 64, columns] = block
        mix = jnp.dot(gates[...], weights[...], preferred_element_type=F32).astype(BF)
        sums = (tokens[part][p].astype(F32) + mix.astype(F32)).astype(BF)
        lanes += squares(sums)
        f = 4 * xt + 2 * ct
        normed[f] = sums[:, :128]
        normed[f + 1] = sums[:, 128:]
        if p == 0 and part == 0:
            resid[...] = sums
    inverse = lax.rsqrt(jnp.sum(lanes, axis=-1, keepdims=True) * (1.0 / 2048) + EPS)
    for f in range(16):
        row = gain[f : f + 1, :]
        normed[f] = (normed[f].astype(F32) * inverse * row).astype(BF)


def add_terms(normed, blocks, orders, acc, fresh):
    place, c = here()
    here_now = {"y": place["y"], "z": place["z"]}
    for weights, base in blocks:
        for i in (0, 2):
            left = []
            for p in (base + i, base + i + 1):
                src = by_core(c, lambda k: source(orders[k], p, here_now))
                left.append(normed[src["z"] * 4 + src["y"]])
            right = jnp.concatenate([weights[i, :704, :], weights[i + 1, :704, :]], axis=-1)
            term = lax.dot_general(
                jnp.concatenate(left, axis=-1), right, NT, preferred_element_type=F32
            )
            if fresh:
                acc[...] = term
                fresh = False
            else:
                acc[...] += term


def early_kernel(normed, *refs):
    firsts, seconds, (gate_acc, up_acc) = refs[:3], refs[3:6], refs[6:]
    bases = (0, 4, 8)
    add_terms(normed, tuple(zip(firsts, bases)), FIRST, gate_acc, True)
    add_terms(normed, tuple(zip(seconds, bases)), SECOND, up_acc, True)


def late_kernel(normed, *refs):
    firsts, seconds, (gate_acc, up_acc, g_scale, u_scale) = refs[:4], refs[4:8], refs[8:12]
    hidden, deep, sums = refs[12:]
    place, c = here()
    here_now = {"y": place["y"], "z": place["z"]}
    for blocks, orders, rows in ((firsts, FIRST, slice(0, LOW)), (seconds, SECOND, slice(LOW, 704))):
        for p in range(16):
            src = by_core(c, lambda k: source(orders[k], p, here_now))
            deep[src["z"] * 4 + src["y"], rows, :] = blocks[p // 4][p % 4, 704:, :]
    sums[0] = gate_acc[...]
    sums[1] = up_acc[...]
    add_terms(normed, ((firsts[3], 12),), FIRST, sums.at[0], False)
    add_terms(normed, ((seconds[3], 12),), SECOND, sums.at[1], False)
    scaled = sums[0] * g_scale[...]
    hidden[...] = (scaled / (1.0 + jnp.exp(-scaled)) * (sums[1] * u_scale[...])).astype(BF)


def down_kernel(mine, part, hidden, deep, sums):
    length = hidden.shape[0] // PARTS
    chosen = slice(part * length, (part + 1) * length)
    place, c = here()
    ct = c if mine else 1 - c
    for xt in range(4):
        f = 4 * xt + 2 * ct
        weights = jnp.concatenate([deep[f], deep[f + 1]], axis=-1)
        term = jnp.dot(hidden[chosen, :], weights, preferred_element_type=F32).astype(BF)

        def rank(k):
            first, second = ALONG[k][1][1], ALONG[k][0][1]
            x = place["x"]
            return jnp.where(
                xt == x,
                0,
                jnp.where(xt == hop(second, x), 1, jnp.where(xt == hop(first, x), 2, 3)),
            )

        r = by_core(ct, rank)
        sums[r, 0] = term[:, :128]
        sums[r, 1] = term[:, 128:]


VMEM = pl.BlockSpec(memory_space=pltpu.VMEM)


def call(kernel, outs, count, flops, scratch=()):
    return pl.pallas_call(
        kernel,
        out_shape=outs,
        in_specs=[VMEM] * (count - 1),
        out_specs=jax.tree.map(lambda _: VMEM, outs),
        scratch_shapes=list(scratch),
        compiler_params=pltpu.CompilerParams(vmem_limit_bytes=10 * 1024 * 1024),
        cost_estimate=pl.CostEstimate(flops=flops, bytes_accessed=1 << 22, transcendentals=0),
    )


def layer(
    tokens,
    pre_gain,
    u_weight,
    u_scale,
    v_weight,
    v_scale,
    group_gain,
    span_weight,
    span_bias,
    out_weight,
    out_scale,
    ffn_gain,
    gate_weight,
    gate_scale,
    up_weight,
    up_scale,
    down_weight,
    down_scale,
):
    shape = jax.ShapeDtypeStruct
    rows = tokens.shape[0]
    tok_own = grown(tokens[None], ALONG, (0, 1))
    tok_other = swapped(tok_own)

    out_scaled = (out_weight.astype(BF).astype(F32) * out_scale).astype(BF)
    deep = (down_weight.astype(BF).astype(F32) * down_scale).astype(BF)
    small = jnp.concatenate([u_weight.T.astype(BF), v_weight.T.astype(BF), out_scaled], axis=0)[None]
    first = jnp.concatenate([gate_weight.T.astype(BF), deep[:LOW]], axis=0)[None]
    second = jnp.concatenate([up_weight.T.astype(BF), deep[LOW:]], axis=0)[None]
    small = grown(small, SMALL, (0, 1, 2, 3))
    pieces = []
    for array, orders in ((first, FIRST), (second, SECOND)):
        array = grown(array, orders, (0, 1))
        got = exchange(array, (orders[0][2], orders[1][2]))
        last = (orders[0][3], orders[1][3])
        pieces.append((array, got, exchange(array, last), exchange(got, last)))
    firsts, seconds = pieces

    message = call(mixer_kernel, shape((1, 1280, 128), BF), 10, 3 * 10**8)(
        tok_own,
        tok_other,
        small,
        pre_gain.reshape(16, 128),
        u_scale.reshape(1, 64),
        v_scale.reshape(1, 64),
        group_gain.reshape(1, 64),
        span_weight,
        span_bias,
    )
    m_own = grown(message, ALONG, (0, 1))
    m_other = swapped(m_own)
    normed, resid = call(
        out_kernel,
        (shape((16, rows, 128), BF), shape((rows, 256), BF)),
        6,
        10**9,
        scratch=[pltpu.VMEM((rows, 512), BF), pltpu.VMEM((512, 256), BF)],
    )(tok_own, tok_other, m_own, m_other, ffn_gain.reshape(16, 128))
    accs = call(
        early_kernel, (shape((rows, 704), F32), shape((rows, 704), F32)), 8, 2 * 10**9
    )(normed, *firsts[:3], *seconds[:3])
    hidden, deep = call(
        late_kernel,
        (shape((rows, 704), BF), shape((16, 704, 128), BF)),
        14,
        10**9,
        scratch=[pltpu.VMEM((2, rows, 704), F32)],
    )(normed, *firsts, *seconds, *accs, gate_scale.reshape(1, 704), up_scale.reshape(1, 704))

    def down(mine, part):
        return call(
            functools.partial(down_kernel, mine, part),
            shape((4, 2, rows // PARTS, 128), BF),
            3,
            75 * 10**7 // PARTS,
        )(hidden, deep)

    theirs = [swapped(down(False, part)) for part in range(PARTS)]
    done = []
    for part in range(PARTS):
        mine, their = down(True, part).astype(F32), theirs[part].astype(F32)
        sent = (mine[2:] + their[2:]).astype(BF)
        got = exchange(sent, (ALONG[0][1], ALONG[1][1])).astype(F32)
        sent = (mine[1] + their[1] + got[1]).astype(BF)
        last = exchange(sent, (ALONG[0][0], ALONG[1][0])).astype(F32)
        ffn = (mine[0] + their[0] + got[0] + last).astype(BF).astype(F32)
        done.append(jnp.concatenate([ffn[0], ffn[1]], axis=-1))
    return (resid.astype(F32) + jnp.concatenate(done, axis=0)).astype(BF)


def solution(mesh):
    torus = Mesh(mesh.devices.reshape(2, 4, 4, 4, 2), AXES)
    seq, fs, tp = ("zh", "zl", "y"), ("zl", "y"), ("x", "c")
    placed = (
        P(seq, tp),
        P(),
        P(fs, tp),
        P(tp),
        P(fs, tp),
        P(tp),
        P(tp),
        P(tp, None, None),
        P(tp, None),
        P(tp, fs),
        P(fs),
        P(),
        P(fs, tp),
        P(tp),
        P(fs, tp),
        P(tp),
        P(tp, fs),
        P(fs),
    )
    return jax.shard_map(layer, mesh=torus, in_specs=placed, out_specs=P(seq, tp), check_vma=False)
```

```python
import functools

import jax
import jax.numpy as jnp
from jax import lax
from jax.experimental import pallas as pl
from jax.experimental.pallas import tpu as pltpu
from jax.sharding import Mesh
from jax.sharding import PartitionSpec as P


EPS = 0.02
BF = jnp.bfloat16
F32 = jnp.float32
NT = (((1,), (1,)), ((), ()))
LOW = 352
PARTS = 2

AXES = ("zh", "zl", "y", "x", "c")
FIRST = (("ye", "yo", "ze", "zo"), ("ze", "zo", "ye", "yo"))
SECOND = (("yo", "ye", "zo", "ze"), ("zo", "ze", "yo", "ye"))
SMALL = (FIRST[1], FIRST[0])
ALONG = (("xe", "xo"), ("xo", "xe"))


def over(kind, v, size):
    if kind == "e":
        return v ^ 1
    return (v + 2 * (v & 1) - 1) % size


def exchange(array, edges):
    pairs = []
    for i in range(256):
        place = {"z": i // 32, "y": i // 8 % 4, "x": i // 2 % 4, "c": i % 2}
        edge = edges[place["c"]]
        if edge == "c":
            place["c"] ^= 1
        else:
            axis = edge[0]
            place[axis] = over(edge[1], place[axis], 8 if axis == "z" else 4)
        j = ((place["z"] * 4 + place["y"]) * 4 + place["x"]) * 2 + place["c"]
        pairs.append((i, j))
    return lax.ppermute(array, AXES, pairs)


def grown(array, orders, steps):
    for s in steps:
        got = exchange(array, (orders[0][s], orders[1][s]))
        array = jnp.concatenate([array, got], axis=0)
    return array


def swapped(array):
    return exchange(array, ("c", "c"))


def hop(kind, v):
    return over(kind, v, 4) if kind == "e" else (v + 2 * (v & 1) - 1) & 3


def source(order, position, place):
    place = dict(place)
    for s in reversed(range(len(order))):
        if position >> s & 1:
            axis = order[s][0]
            place[axis] = hop(order[s][1], place[axis])
    return place


def position(order, place, target):
    found = 0
    for axis in target:
        kinds = [(s, e[1]) for s, e in enumerate(order) if e[0] == axis]
        here, there = place[axis], target[axis]
        odd = ((there ^ here) >> 1) & 1
        if kinds[1][1] == "o":
            even = (jnp.where(odd == 1, hop("o", here), here) ^ there) & 1
        else:
            even = (jnp.where(odd == 1, hop("o", there), there) ^ here) & 1
        for s, kind in kinds:
            found = found + ((odd if kind == "o" else even) << s)
    return found


def by_core(c, of):
    zero, one = of(0), of(1)
    if isinstance(zero, dict):
        return {a: jnp.where(c == 0, zero[a], one[a]) for a in zero}
    return jnp.where(c == 0, zero, one)


def squares(values):
    wide = values.astype(F32)
    wide = wide * wide
    return wide[:, :128] + wide[:, 128:]


def here():
    return {"x": lax.axis_index("x"), "y": lax.axis_index("y"), "z": lax.axis_index("zl")}, lax.axis_index("c")


def blocks_of():
    place, c = here()
    for p in range(4):
        for part in range(2):
            ct = c if part == 0 else 1 - c
            yield p, part, by_core(ct, lambda k: source(ALONG[k], p, {"x": place["x"]})["x"]), ct


def mixer_kernel(
    own, other, near, far, gain, u_scale, v_scale, group_gain, span, bias, message, small
):
    place, c = here()
    tokens = (own, other)
    for p in range(8):
        small[p] = near[p]
        small[8 + p] = far[p]
    lanes = jnp.zeros((own.shape[1], 128), F32)
    for p in range(4):
        for part in range(2):
            lanes += squares(tokens[part][p])
    inverse = lax.rsqrt(jnp.sum(lanes, axis=-1, keepdims=True) * (1.0 / 2048) + EPS)
    sums = jnp.zeros((own.shape[1], 128), F32)
    for p, part, xt, ct in blocks_of():
        row = jnp.concatenate(
            [gain[pl.ds(4 * xt + 2 * ct, 1), :], gain[pl.ds(4 * xt + 2 * ct + 1, 1), :]], axis=-1
        )
        normed = (tokens[part][p].astype(F32) * inverse * row).astype(BF)
        pieces = []
        for h in range(2):
            target = {"y": 2 * ct + h, "z": xt}
            pieces.append(small[by_core(c, lambda k: position(SMALL[k], place, target)), :128, :])
        weights = jnp.concatenate(pieces, axis=-1)
        sums += lax.dot_general(normed, weights, NT, preferred_element_type=F32)
    acts = jax.nn.gelu(sums * jnp.concatenate([u_scale[...], v_scale[...]], axis=-1))
    u_act = acts[:, :64]
    v_act = acts[:, 64:]
    centred = v_act - jnp.mean(v_act, axis=-1, keepdims=True)
    spread = jnp.mean(centred * centred, axis=-1, keepdims=True)
    v_norm = (centred * lax.rsqrt(spread + EPS) * group_gain[...]).astype(BF)
    t = lax.broadcasted_iota(jnp.int32, (128, 128), 0)
    s = lax.broadcasted_iota(jnp.int32, (128, 128), 1)
    for p in range(16):
        message[0, 64 * p : 64 * p + 64, :] = small[p, 128:, :]
    lower = jnp.where(s <= t, span[0].astype(F32), 0.0).astype(BF)
    level = jnp.sum(jnp.where(s == t, bias[...], 0.0), axis=-1, keepdims=True)
    for n in range(own.shape[1] // 128):
        rows = slice(n * 128, (n + 1) * 128)
        mixed = jnp.dot(lower, v_norm[rows], preferred_element_type=F32) + level
        low, side = 1024 + n % 2 * 128, 64 * (n // 2)
        message[0, low : low + 128, side : side + 64] = (u_act[rows] * mixed).astype(BF)


def out_kernel(own, other, m_own, m_other, gain, normed, resid, gates, weights):
    place, c = here()
    tokens = (own, other)
    for p in range(4):
        for part, message in enumerate((m_own, m_other)):
            side = 256 * part + 64 * p
            gates[:256, side : side + 64] = message[p, 1024:, :64]
            gates[256:, side : side + 64] = message[p, 1024:, 64:]
    lanes = jnp.zeros((own.shape[1], 128), F32)
    for p, part, xt, ct in blocks_of():
        for h in range(2):
            target = {"y": 2 * ct + h, "z": xt}
            mine = by_core(c, lambda k: position(SMALL[k], place, target))
            theirs = by_core(1 - c, lambda k: position(SMALL[k], place, target))
            columns = slice(128 * h, 128 * h + 128)
            for j in range(4):
                for base, message, found in ((0, m_own, mine), (256, m_other, theirs)):
                    block = message[j, pl.ds(pl.multiple_of(found * 64, 64), 64), :]
                    weights[base + 64 * j : base + 64 * j + 64, columns] = block
        mix = jnp.dot(gates[...], weights[...], preferred_element_type=F32).astype(BF)
        sums = (tokens[part][p].astype(F32) + mix.astype(F32)).astype(BF)
        lanes += squares(sums)
        f = 4 * xt + 2 * ct
        normed[f] = sums[:, :128]
        normed[f + 1] = sums[:, 128:]
        if p == 0 and part == 0:
            resid[...] = sums
    inverse = lax.rsqrt(jnp.sum(lanes, axis=-1, keepdims=True) * (1.0 / 2048) + EPS)
    for f in range(16):
        row = gain[f : f + 1, :]
        normed[f] = (normed[f].astype(F32) * inverse * row).astype(BF)


def add_terms(normed, blocks, orders, acc, fresh):
    place, c = here()
    here_now = {"y": place["y"], "z": place["z"]}
    for weights, base in blocks:
        for i in (0, 2):
            left = []
            for p in (base + i, base + i + 1):
                src = by_core(c, lambda k: source(orders[k], p, here_now))
                left.append(normed[src["z"] * 4 + src["y"]])
            right = jnp.concatenate([weights[i, :704, :], weights[i + 1, :704, :]], axis=-1)
            term = lax.dot_general(
                jnp.concatenate(left, axis=-1), right, NT, preferred_element_type=F32
            )
            if fresh:
                acc[...] = term
                fresh = False
            else:
                acc[...] += term


def early_kernel(normed, *refs):
    firsts, seconds, (gate_acc, up_acc) = refs[:3], refs[3:6], refs[6:]
    bases = (0, 4, 8)
    add_terms(normed, tuple(zip(firsts, bases)), FIRST, gate_acc, True)
    add_terms(normed, tuple(zip(seconds, bases)), SECOND, up_acc, True)


def late_kernel(normed, *refs):
    firsts, seconds, (gate_acc, up_acc, g_scale, u_scale) = refs[:4], refs[4:8], refs[8:12]
    hidden, deep, sums = refs[12:]
    place, c = here()
    here_now = {"y": place["y"], "z": place["z"]}
    for blocks, orders, rows in ((firsts, FIRST, slice(0, LOW)), (seconds, SECOND, slice(LOW, 704))):
        for p in range(16):
            src = by_core(c, lambda k: source(orders[k], p, here_now))
            deep[src["z"] * 4 + src["y"], rows, :] = blocks[p // 4][p % 4, 704:, :]
    sums[0] = gate_acc[...]
    sums[1] = up_acc[...]
    add_terms(normed, ((firsts[3], 12),), FIRST, sums.at[0], False)
    add_terms(normed, ((seconds[3], 12),), SECOND, sums.at[1], False)
    scaled = sums[0] * g_scale[...]
    hidden[...] = (scaled / (1.0 + jnp.exp(-scaled)) * (sums[1] * u_scale[...])).astype(BF)


def down_kernel(mine, part, hidden, deep, sums):
    length = hidden.shape[0] // PARTS
    chosen = slice(part * length, (part + 1) * length)
    place, c = here()
    ct = c if mine else 1 - c
    for xt in range(4):
        f = 4 * xt + 2 * ct
        weights = jnp.concatenate([deep[f], deep[f + 1]], axis=-1)
        term = jnp.dot(hidden[chosen, :], weights, preferred_element_type=F32).astype(BF)

        def rank(k):
            first, second = ALONG[k][1][1], ALONG[k][0][1]
            x = place["x"]
            return jnp.where(
                xt == x,
                0,
                jnp.where(xt == hop(second, x), 1, jnp.where(xt == hop(first, x), 2, 3)),
            )

        r = by_core(ct, rank)
        sums[r, 0] = term[:, :128]
        sums[r, 1] = term[:, 128:]


VMEM = pl.BlockSpec(memory_space=pltpu.VMEM)


def call(kernel, outs, count, flops, scratch=()):
    return pl.pallas_call(
        kernel,
        out_shape=outs,
        in_specs=[VMEM] * (count - 1),
        out_specs=jax.tree.map(lambda _: VMEM, outs),
        scratch_shapes=list(scratch),
        compiler_params=pltpu.CompilerParams(vmem_limit_bytes=10 * 1024 * 1024),
        cost_estimate=pl.CostEstimate(flops=flops, bytes_accessed=1 << 22, transcendentals=0),
    )


def layer(
    tokens,
    pre_gain,
    u_weight,
    u_scale,
    v_weight,
    v_scale,
    group_gain,
    span_weight,
    span_bias,
    out_weight,
    out_scale,
    ffn_gain,
    gate_weight,
    gate_scale,
    up_weight,
    up_scale,
    down_weight,
    down_scale,
):
    shape = jax.ShapeDtypeStruct
    rows = tokens.shape[0]
    tok_own = grown(tokens[None], ALONG, (0, 1))
    tok_other = swapped(tok_own)

    out_scaled = (out_weight.astype(BF).astype(F32) * out_scale).astype(BF)
    deep = (down_weight.astype(BF).astype(F32) * down_scale).astype(BF)
    small = jnp.concatenate([u_weight.T.astype(BF), v_weight.T.astype(BF), out_scaled], axis=0)[None]
    first = jnp.concatenate([gate_weight.T.astype(BF), deep[:LOW]], axis=0)[None]
    second = jnp.concatenate([up_weight.T.astype(BF), deep[LOW:]], axis=0)[None]
    small = grown(small, SMALL, (0, 1, 2))
    small_far = exchange(small, (SMALL[0][3], SMALL[1][3]))
    pieces = []
    for array, orders in ((first, FIRST), (second, SECOND)):
        array = grown(array, orders, (0, 1))
        got = exchange(array, (orders[0][2], orders[1][2]))
        last = (orders[0][3], orders[1][3])
        pieces.append((array, got, exchange(array, last), exchange(got, last)))
    firsts, seconds = pieces

    message = call(
        mixer_kernel,
        shape((1, 1280, 128), BF),
        11,
        3 * 10**8,
        scratch=[pltpu.VMEM((16, 192, 128), BF)],
    )(
        tok_own,
        tok_other,
        small,
        small_far,
        pre_gain.reshape(16, 128),
        u_scale.reshape(1, 64),
        v_scale.reshape(1, 64),
        group_gain.reshape(1, 64),
        span_weight,
        span_bias,
    )
    m_own = grown(message, ALONG, (0, 1))
    m_other = swapped(m_own)
    normed, resid = call(
        out_kernel,
        (shape((16, rows, 128), BF), shape((rows, 256), BF)),
        6,
        10**9,
        scratch=[pltpu.VMEM((rows, 512), BF), pltpu.VMEM((512, 256), BF)],
    )(tok_own, tok_other, m_own, m_other, ffn_gain.reshape(16, 128))
    accs = call(
        early_kernel, (shape((rows, 704), F32), shape((rows, 704), F32)), 8, 2 * 10**9
    )(normed, *firsts[:3], *seconds[:3])
    hidden, deep = call(
        late_kernel,
        (shape((rows, 704), BF), shape((16, 704, 128), BF)),
        14,
        10**9,
        scratch=[pltpu.VMEM((2, rows, 704), F32)],
    )(normed, *firsts, *seconds, *accs, gate_scale.reshape(1, 704), up_scale.reshape(1, 704))

    def down(mine, part):
        return call(
            functools.partial(down_kernel, mine, part),
            shape((4, 2, rows // PARTS, 128), BF),
            3,
            75 * 10**7 // PARTS,
        )(hidden, deep)

    theirs = [swapped(down(False, part)) for part in range(PARTS)]
    done = []
    for part in range(PARTS):
        mine, their = down(True, part).astype(F32), theirs[part].astype(F32)
        sent = (mine[2:] + their[2:]).astype(BF)
        got = exchange(sent, (ALONG[0][1], ALONG[1][1])).astype(F32)
        sent = (mine[1] + their[1] + got[1]).astype(BF)
        last = exchange(sent, (ALONG[0][0], ALONG[1][0])).astype(F32)
        ffn = (mine[0] + their[0] + got[0] + last).astype(BF).astype(F32)
        done.append(jnp.concatenate([ffn[0], ffn[1]], axis=-1))
    return (resid.astype(F32) + jnp.concatenate(done, axis=0)).astype(BF)


def solution(mesh):
    torus = Mesh(mesh.devices.reshape(2, 4, 4, 4, 2), AXES)
    seq, fs, tp = ("zh", "zl", "y"), ("zl", "y"), ("x", "c")
    placed = (
        P(seq, tp),
        P(),
        P(fs, tp),
        P(tp),
        P(fs, tp),
        P(tp),
        P(tp),
        P(tp, None, None),
        P(tp, None),
        P(tp, fs),
        P(fs),
        P(),
        P(fs, tp),
        P(tp),
        P(fs, tp),
        P(tp),
        P(tp, fs),
        P(fs),
    )
    return jax.shard_map(layer, mesh=torus, in_specs=placed, out_specs=P(seq, tp), check_vma=False)
```
